32 devices in a mesh: rep: 2 (over x), fs: 8 (over z, y), tp: 2 (over core).
Axes of the slice: x: 2, y: 2, z: 4, core: 2. Of those that a mesh axis runs over, the one named last changes fastest.
Arguments:
- tokens: bfloat16 [16, 512, 2048], P(('rep', 'fs'), 'tp'), may hold values from -6 to 6
- norm_first: bfloat16 [2048], replicated, may hold values from 0.099609375 to 1.8984375
- norm_mixer: bfloat16 [2048], replicated, may hold values from 0.099609375 to 1.8984375
- norm_second: bfloat16 [2048], replicated, may hold values from 0.099609375 to 1.8984375
- ffn_gate: bfloat16 [2048, 2816], P('fs', 'tp'), may hold values from -0.125 to 0.125
- ffn_up: bfloat16 [2048, 2816], P('fs', 'tp'), may hold values from -0.125 to 0.125
- ffn_down: bfloat16 [2816, 2048], P('tp', 'fs'), may hold values from -0.109375 to 0.109375
- conv_value: bfloat16 [2048, 512], P('fs', 'tp'), may hold values from -0.125 to 0.125
- conv_gate: bfloat16 [2048, 512], P('fs', 'tp'), may hold values from -0.125 to 0.125
- depthwise: bfloat16 [31, 512], P(None, 'tp'), may hold values from -1.5 to 1.5
- conv_gain: bfloat16 [512], P('tp'), may hold values from 0.099609375 to 1.8984375
- conv_out: bfloat16 [512, 2048], P('tp', 'fs'), may hold values from -0.25 to 0.25
Outputs:
- mixed: bfloat16 [16, 512, 2048], P(('rep', 'fs'), 'tp')
The draws below stay inside these ranges and needn't reach their ends.
All inputs are finite; a program needn't handle non-finite values.
Results may differ from the reference program's by a relative error of at most 0.0095.
Values may be sent and summed in bfloat16 or wider, within the bound.
A program may use at most 128 MiB of HBM per device.

```python
import jax
import jax.numpy as jnp
from jax import lax

D = 2048
FF = 2816
CONV = 512
KSIZE = 31
LEN = 512
SEQS = 16
N_TP = 2


def draw_depthwise(key, part):
    first, second, third = jax.random.split(jax.random.fold_in(key, 7), 3)
    base = jnp.clip(jax.random.normal(first, (KSIZE, CONV), jnp.float32), -3.0, 3.0) * KSIZE ** (-0.5)
    flipped = jax.random.randint(second, (), 0, 2)
    channel = jnp.arange(CONV)
    upper = (channel >= CONV // 2).astype(jnp.int32)
    factor = jnp.where(upper == flipped, 0.5, 1.6)
    jitter = jnp.exp(jax.random.uniform(third, (CONV,), jnp.float32, -0.35, 0.35))
    return (base * (factor * jitter)[None, :]).astype(jnp.bfloat16)


def block_levels(rng, extent, cuts, least, high):
    def one(axis_at, shards_of):
        heights = jax.random.uniform(jax.random.fold_in(jax.random.fold_in(rng, 6), axis_at), (shards_of,), jnp.float32, least / len(cuts), high / len(cuts))
        return jnp.repeat(jnp.exp(heights), extent[axis_at] // shards_of).reshape((-1,) + (1,) * (len(extent) - axis_at - 1))

    loudness = one(*cuts[0])
    for cut in cuts[1:]:
        loudness = loudness * one(*cut)
    return loudness


def gaussian(own_key, shape, scale, bound, cuts=(), dtype=jnp.bfloat16):
    result = jax.random.normal(own_key, shape, jnp.float32) * scale
    if len(cuts) > 0:
        result = block_levels(own_key, shape, cuts, -0.22, 0.18) * result
    return jnp.clip(result, min=-bound, max=bound).astype(dtype)


def setup_inputs(seed: int = 0) -> dict:
    arg_keys = jax.random.split(jax.random.key(seed), 13)
    tokens = gaussian(arg_keys[0], (SEQS, LEN, D), 1.0, 6.0, ((0, 16), (1, 2)))
    norm_first = jnp.clip(1.0 + 0.18 * jax.random.normal(arg_keys[1], (D,), jnp.float32), 0.099609375, 1.8984375).astype(jnp.bfloat16)
    norm_mixer = jnp.clip(1.0 + 0.18 * jax.random.normal(arg_keys[2], (D,), jnp.float32), 0.099609375, 1.8984375).astype(jnp.bfloat16)
    norm_second = jnp.clip(1.0 + 0.18 * jax.random.normal(arg_keys[3], (D,), jnp.float32), 0.099609375, 1.8984375).astype(jnp.bfloat16)
    ffn_gate = gaussian(arg_keys[4], (D, FF), D ** -0.5, 0.125, ((0, 8), (1, 2)))
    ffn_up = gaussian(arg_keys[5], (D, FF), D ** -0.5, 0.125, ((0, 8), (1, 2)))
    ffn_down = gaussian(arg_keys[6], (FF, D), FF ** -0.5, 0.109375, ((0, 2), (1, 8)))
    conv_value = gaussian(arg_keys[7], (D, CONV), D ** -0.5, 0.125, ((0, 8), (1, 2)))
    conv_gate = gaussian(arg_keys[8], (D, CONV), D ** -0.5, 0.125, ((0, 8), (1, 2)))
    depthwise = draw_depthwise(jax.random.fold_in(arg_keys[12], 71), 0)
    conv_gain = jnp.clip(1.0 + 0.18 * jax.random.normal(arg_keys[10], (CONV,), jnp.float32), 0.099609375, 1.8984375).astype(jnp.bfloat16)
    conv_out = gaussian(arg_keys[11], (CONV, D), CONV ** -0.5, 0.25, ((0, 2), (1, 8)))
    return {"tokens": tokens, "norm_first": norm_first, "norm_mixer": norm_mixer, "norm_second": norm_second, "ffn_gate": ffn_gate, "ffn_up": ffn_up, "ffn_down": ffn_down, "conv_value": conv_value, "conv_gate": conv_gate, "depthwise": depthwise, "conv_gain": conv_gain, "conv_out": conv_out}


ROW_EPS = 0.05
CHAN_EPS = 0.02

def rms_rows(stream, gain_vec):
    square_mean = lax.optimization_barrier(jnp.mean(stream * stream, axis=-1, keepdims=True))
    return (stream * lax.rsqrt(square_mean + ROW_EPS) * gain_vec.astype(jnp.float32)).astype(jnp.bfloat16)

def block_sum(left, right, blocks):
    width = left.shape[1] // blocks
    running = jnp.zeros((left.shape[0], right.shape[1]), jnp.float32)
    for block in range(blocks):
        partial_value = jnp.dot(left[:, block * width:(block + 1) * width], right[block * width:(block + 1) * width], preferred_element_type=jnp.float32)
        running = running + lax.optimization_barrier(partial_value.astype(jnp.bfloat16)).astype(jnp.float32)
    return running

def causal_taps(glu, kernel):
    length = glu.shape[0]
    padded = jnp.pad(glu, ((KSIZE - 1, 0), (0, 0)))
    output = jnp.zeros_like(glu)
    for tap_index in range(KSIZE):
        output = output + padded[tap_index:tap_index + length] * kernel[tap_index]
    return output

def reference(tokens, norm_first, norm_mixer, norm_second, ffn_gate, ffn_up, ffn_down, conv_value, conv_gate, depthwise, conv_gain, conv_out):

    def feed(normed):
        gate_rows = jnp.dot(normed, ffn_gate, preferred_element_type=jnp.float32)
        up_rows = jnp.dot(normed, ffn_up, preferred_element_type=jnp.float32)
        hidden = (jax.nn.silu(gate_rows) * up_rows).astype(jnp.bfloat16)
        return block_sum(hidden, ffn_down, N_TP)

    def one_sequence(sequence):
        stream = sequence.astype(jnp.float32)
        stream = stream + 0.5 * feed(rms_rows(stream, norm_first))
        normed = rms_rows(stream, norm_mixer)
        values = jnp.dot(normed, conv_value, preferred_element_type=jnp.float32)
        gates = jnp.dot(normed, conv_gate, preferred_element_type=jnp.float32)
        glu = values * jax.nn.sigmoid(gates)
        conv = causal_taps(glu, depthwise.astype(jnp.float32))
        average = lax.optimization_barrier(jnp.mean(conv, axis=-1, keepdims=True))
        centred = conv - average
        spread = lax.optimization_barrier(jnp.mean(centred * centred, axis=-1, keepdims=True))
        activated = jax.nn.silu(centred * lax.rsqrt(spread + CHAN_EPS) * conv_gain.astype(jnp.float32)).astype(jnp.bfloat16)
        stream = stream + block_sum(activated, conv_out, N_TP)
        stream = stream + 0.5 * feed(rms_rows(stream, norm_second))
        return stream.astype(jnp.bfloat16)
    return lax.map(one_sequence, tokens)
```

```python
import functools

import jax
import jax.numpy as jnp
from jax import lax
from jax.experimental import pallas as pl
from jax.experimental.pallas import tpu as pltpu
from jax.sharding import PartitionSpec as P

ROW_EPS = 0.05
CHAN_EPS = 0.02
MESH = pl.DeviceIdType.MESH
LEAD = 1.5
LAG = 1.6


def rms_rows(stream, gain_vec):
    square_mean = jnp.mean(stream * stream, axis=-1, keepdims=True)
    return (stream * lax.rsqrt(square_mean + ROW_EPS) * gain_vec.astype(jnp.float32)).astype(
        jnp.bfloat16
    )


def swap(value):
    size = lax.axis_size("tp")
    return lax.ppermute(value, "tp", [(i, size - 1 - i) for i in range(size)])


def widen(normed):
    return jnp.concatenate([normed, swap(normed)])


def narrow(partial_value):
    rounded = partial_value.astype(jnp.bfloat16)
    half = rounded.shape[0] // 2
    return rounded[:half].astype(jnp.float32) + swap(rounded[half:]).astype(jnp.float32)


def reorder(rows):
    half = rows.shape[0] // 2
    flipped = jnp.concatenate([rows[half:], rows[:half]])
    return jnp.where(lax.axis_index("tp") == 0, rows, flipped)


def place():
    fs = lax.axis_index("fs")
    return lax.axis_index("rep"), lax.rem(fs, 2), fs // 2


class Gather:
    def __init__(self, depth, ins, slots, local_sems, recv_sems, send_sems):
        self.depth = depth
        self.ins, self.slots = ins, slots
        self.local_sems, self.recv_sems, self.send_sems = local_sems, recv_sems, send_sems
        self.x, self.y, self.z = place()

    def targets(self):
        other_x = {"rep": 1 - self.x}
        other_y = {"fs": self.z * 2 + 1 - self.y}
        up = {"fs": (self.z + 1) * 2 + self.y}
        down = {"fs": (self.z - 1) * 2 + self.y}
        return up, down, other_x, other_y

    def barrier(self):
        barrier = pltpu.get_barrier_semaphore()
        up, down, other_x, other_y = self.targets()
        has_up, has_down = self.z + 1 < self.depth, self.z > 0
        for target in (other_x, other_y):
            pl.semaphore_signal(barrier, inc=1, device_id=target, device_id_type=MESH)

        @pl.when(has_up)
        def _():
            pl.semaphore_signal(barrier, inc=1, device_id=up, device_id_type=MESH)

        @pl.when(has_down)
        def _():
            pl.semaphore_signal(barrier, inc=1, device_id=down, device_id_type=MESH)

        peers = 2 + has_up.astype(jnp.int32) + has_down.astype(jnp.int32)
        pl.semaphore_wait(barrier, peers)

    def local(self, m, c):
        k = self.z * 2 + self.y
        return pltpu.make_async_copy(
            self.ins[m].at[c], self.slots[m].at[k, c], self.local_sems[m].at[c]
        )

    def copy(self, m, c, k, way):
        piece = self.slots[m].at[k, c]
        return pltpu.make_async_remote_copy(
            src_ref=piece,
            dst_ref=piece,
            send_sem=self.send_sems[m].at[way, k, c],
            recv_sem=self.recv_sems[m].at[k, c],
            device_id=self.targets()[way],
            device_id_type=MESH,
        )

    def routes(self, m, c, side, d):
        x, y, z = self.x, self.y, self.z
        home = x == lax.rem(c, 2)
        has_up, has_down = z + 1 < self.depth, z > 0
        off = z < 0
        if side == "far_below":
            return (z - d) * 2 + 1 - y, z - d >= 0, (off, off, home, off)
        if side == "far_above":
            return (z + d) * 2 + 1 - y, z + d < self.depth, (off, off, home, off)
        if side == "own":
            return z * 2 + y, z >= 0, (has_up, has_down, off, home)
        if side == "below":
            return (z - d) * 2 + y, z - d >= 0, (has_up, off, off, home)
        return (z + d) * 2 + y, z + d < self.depth, (off, has_down, off, home)

    def event(self, m, side, d, finish=False):
        def step(c, carry):
            k, present, sends = self.routes(m, c, side, d)

            @pl.when(present)
            def _():
                if not finish:
                    if side == "own":
                        self.local(m, c).wait()
                    else:
                        self.copy(m, c, k, 2).wait_recv()
                for way, wanted in enumerate(sends):

                    @pl.when(wanted)
                    def _(way=way):
                        if finish:
                            self.copy(m, c, k, way).wait_send()
                        else:
                            self.copy(m, c, k, way).start()

            return carry

        lax.fori_loop(0, self.ins[m].shape[0], step, 0)

    def start_local(self):
        for m in range(len(self.ins)):

            def step(c, carry, m=m):
                self.local(m, c).start()
                return carry

            lax.fori_loop(0, self.ins[m].shape[0], step, 0)

    def plan(self):
        events = []
        span = self.depth - 1
        for m in range(len(self.ins)):
            start = m * span
            events.append((start - LEAD, m, "own", 0))
            events.append((start + LAG, m, "far_below", 0))
            for d in range(1, self.depth):
                events.append((start + d, m, "below", d))
                events.append((start + d, m, "above", d))
                events.append((start + d + LAG, m, "far_below", d))
                events.append((start + d + LAG, m, "far_above", d))
        return sorted(events, key=lambda event: event[0])

    def finish(self):
        for _, m, side, d in self.plan():
            self.event(m, side, d, finish=True)


def gather_kernel(depth, count, *refs):
    ins, slots = refs[:count], refs[count : 2 * count]
    sems = refs[2 * count :]
    gather = Gather(depth, ins, slots, sems[:count], sems[count : 2 * count], sems[2 * count :])
    gather.start_local()
    gather.barrier()
    for _, m, side, d in gather.plan():
        gather.event(m, side, d)
    gather.finish()


def gather_all(blocks):
    total = lax.axis_size("fs")
    count = len(blocks)
    outs = [jax.ShapeDtypeStruct((total, *b.shape), b.dtype) for b in blocks]
    dma = pltpu.SemaphoreType.DMA
    return pl.pallas_call(
        functools.partial(gather_kernel, total // 2, count),
        out_shape=outs,
        in_specs=[pl.BlockSpec(memory_space=pl.ANY)] * count,
        out_specs=[pl.BlockSpec(memory_space=pltpu.VMEM)] * count,
        scratch_shapes=[dma((b.shape[0],)) for b in blocks]
        + [dma((total, b.shape[0])) for b in blocks]
        + [dma((4, total, b.shape[0])) for b in blocks],
        compiler_params=pltpu.CompilerParams(
            collective_id=0, has_side_effects=True, vmem_limit_bytes=48 * 2**20
        ),
        name="gather_all",
    )(*blocks)


def hidden_units(gathered, whole_gate, whole_up):
    gate_rows = jnp.dot(gathered, whole_gate, preferred_element_type=jnp.float32)
    up_rows = jnp.dot(gathered, whole_up, preferred_element_type=jnp.float32)
    return (jax.nn.silu(gate_rows) * up_rows).astype(jnp.bfloat16)


def columns_of(blocks):
    return blocks.transpose(1, 0, 2).reshape(blocks.shape[1], -1)


def causal_taps(glu, kernel):
    length = glu.shape[0]
    taps = kernel.shape[0]
    padded = jnp.pad(glu, ((taps - 1, 0), (0, 0)))
    output = jnp.zeros_like(glu)
    for tap_index in range(taps):
        output = output + padded[tap_index : tap_index + length] * kernel[tap_index]
    return output


def chunked(block, pieces):
    return block.reshape(pieces, block.shape[0] // pieces, block.shape[1])


def shards(
    tokens,
    norm_first,
    norm_mixer,
    norm_second,
    ffn_gate,
    ffn_up,
    ffn_down,
    conv_value,
    conv_gate,
    depthwise,
    conv_gain,
    conv_out,
):
    width = tokens.shape[-1]
    stream = tokens.reshape(-1, width).astype(jnp.float32)
    first_rows = widen(rms_rows(stream, norm_first))
    small = jnp.concatenate([conv_value, conv_gate, conv_out.reshape(-1, conv_value.shape[1])])
    gate, up, down, small_all = gather_all(
        [chunked(ffn_gate, 4), chunked(ffn_up, 4), chunked(ffn_down, 4), chunked(small, 2)]
    )
    whole_gate = gate.reshape(-1, gate.shape[-1])
    whole_up = up.reshape(-1, up.shape[-1])
    whole_down = columns_of(down.reshape(down.shape[0], -1, down.shape[-1]))
    total = small_all.shape[0]
    small_all = small_all.reshape(total, -1, small_all.shape[-1])
    rows = conv_value.shape[0]
    channels_here = conv_value.shape[1]
    whole_value = small_all[:, :rows].reshape(-1, channels_here)
    whole_conv_gate = small_all[:, rows : 2 * rows].reshape(-1, channels_here)
    whole_out = columns_of(small_all[:, 2 * rows :].reshape(total, *conv_out.shape))

    hidden = hidden_units(first_rows, whole_gate, whole_up)
    stream = stream + 0.5 * narrow(jnp.dot(hidden, whole_down, preferred_element_type=jnp.float32))
    gathered = widen(rms_rows(stream, norm_mixer))
    values = jnp.dot(gathered, whole_value, preferred_element_type=jnp.float32)
    gates = jnp.dot(gathered, whole_conv_gate, preferred_element_type=jnp.float32)
    glu = reorder(values * jax.nn.sigmoid(gates))
    conv = causal_taps(glu, depthwise.astype(jnp.float32))
    channels = conv.shape[1] * lax.axis_size("tp")
    sums, squares = lax.psum((jnp.sum(conv, axis=1), jnp.sum(conv * conv, axis=1)), "tp")
    average = sums / channels
    spread = jnp.maximum(squares / channels - average * average, 0.0)
    centred = conv - average[:, None]
    activated = jax.nn.silu(
        centred * lax.rsqrt(spread[:, None] + CHAN_EPS) * conv_gain.astype(jnp.float32)
    ).astype(jnp.bfloat16)
    stream = stream + narrow(jnp.dot(reorder(activated), whole_out, preferred_element_type=jnp.float32))
    second_rows = widen(rms_rows(stream, norm_second))
    second_hidden = hidden_units(second_rows, whole_gate, whole_up)
    stream = stream + 0.5 * narrow(jnp.dot(second_hidden, whole_down, preferred_element_type=jnp.float32))
    return stream.astype(jnp.bfloat16).reshape(tokens.shape)


def solution(mesh):
    in_specs = (
        P(("rep", "fs"), "tp", None),
        P(),
        P(),
        P(),
        P("fs", "tp"),
        P("fs", "tp"),
        P("tp", "fs"),
        P("fs", "tp"),
        P("fs", "tp"),
        P(None, "tp"),
        P("tp"),
        P("tp", "fs"),
    )
    out_specs = P(("rep", "fs"), "tp", None)
    return jax.shard_map(shards, mesh=mesh, in_specs=in_specs, out_specs=out_specs, check_vma=False)
```
